32 devices in a mesh: grp: 2 (over y), sp: 8 (over z, core), tp: 2 (over x).
Axes of the slice: x: 2, y: 2, z: 4, core: 2. Of those that a mesh axis runs over, the one named last changes fastest.
Arguments:
- tokens: bfloat16 [12288, 2048], P(('grp', 'sp'), 'tp'), parts along dimension 0, may hold values from -4000 to 4000
- gain: float32 [2048], replicated, may hold values from 0.1 to 1.9
- w_query: bfloat16 [2048, 1024], P('sp', 'tp'), may hold values from -1 to 1
- w_key: bfloat16 [2048, 256], P('sp', 'tp'), may hold values from -1 to 1
- w_value: bfloat16 [2048, 256], P('sp', 'tp'), may hold values from -0.125 to 0.125
- w_input: bfloat16 [2048, 1024], P('sp', 'tp'), may hold values from -0.125 to 0.125
- w_bgate: bfloat16 [2048, 1024], P('sp', 'tp'), may hold values from -0.125 to 0.125
- w_cgate: bfloat16 [2048, 1024], P('sp', 'tp'), may hold values from -0.125 to 0.125
- w_attn_out: bfloat16 [1024, 2048], P('sp', 'tp'), may hold values from -2 to 2
- w_conv_out: bfloat16 [1024, 2048], P('sp', 'tp'), may hold values from -0.1875 to 0.1875
- sink_logit: float32 [16], P('tp'), may hold values from 0 to 5
- taps: float32 [3, 1024], P(None, 'tp'), may hold values from -3.5 to 3.5
- conv_bias: float32 [1024], P('tp'), may hold values from -4 to 4
- documents: int32 [12288], P(('grp', 'sp')), parts along dimension 0, may hold values from 0 to 3, never falling along the last dimension, each value on 1 to 3072 neighbouring positions
Outputs:
- mixed: bfloat16 [12288, 2048], P(('grp', 'sp'), 'tp'), parts along dimension 0
The draws below stay inside these ranges and needn't reach their ends.
There are 2 independent parts, one for each index of `grp`. The reference program is written for one: setup_inputs(seed, part) draws one part's arguments, and reference() takes and returns one part's arrays. A program takes and returns all parts, laid end to end along the dimension named above; an argument that names none is the same for every part. Nothing has to cross between parts.
All inputs are finite; a program needn't handle non-finite values.
Results may differ from the reference program's by a relative error of at most 0.013.
The reference program's roundings to bfloat16 on the way (of `scaled`, `weight`, `attended`, `carried` and `convolved`) count: a program that leaves them out, or rounds other values in their place, can miss the bound.
Values may be sent and summed in bfloat16 or wider, within the bound.
No kernel may reach another device: no remote copies, remote signals or barrier semaphores. Data moves between devices by JAX's collectives and lax.ppermute only.
A program may use at most 64 MiB of HBM per device.

```python
import math
import jax
import jax.numpy as jnp
import numpy as np
from jax import lax

D = 2048
Q_HEADS = 16
KV_HEADS = 4
HEAD_DIM = 64
CW = 1024
WINDOW = 128
TOK_DEV = 768
QW = 1024
KVW = 256
TOKENS = 6144
DOCS = 4


def draw_tokens(key, part):
    f32 = jnp.float32
    base = jnp.clip(jax.random.normal(jax.random.fold_in(key, 11), (TOKENS, D), f32), -6.0, 6.0)
    columns = jnp.exp(jax.random.uniform(jax.random.fold_in(key, 12), (D,), f32, 0.0, jnp.log(10.0)))
    order = jax.random.permutation(jax.random.fold_in(key, 13), 4).astype(f32)
    blocks = jnp.power(3.0, order / 3.0)
    block_of = (jnp.arange(D) // (D // 4)).astype(jnp.int32)
    columns = columns * blocks[block_of]
    rows = jnp.exp(jax.random.uniform(jax.random.fold_in(key, 14), (TOKENS, 1), f32, 0.0, jnp.log(10.0)))
    values = base * columns[None, :] * rows
    return values.astype(jnp.bfloat16)


def query_parts(key):
    f32 = jnp.float32
    base = jnp.clip(jax.random.normal(jax.random.fold_in(key, 101), (D, Q_HEADS * HEAD_DIM), f32), -6.0, 6.0) * D ** (-0.5)
    return base


def draw_w_query(key, part):
    base = query_parts(key)
    values = base
    return jnp.clip(values, -1.0, 1.0).astype(jnp.bfloat16)


def draw_w_key(key, part):
    f32 = jnp.float32
    values = jnp.clip(jax.random.normal(jax.random.fold_in(key, 202), (D, KV_HEADS * HEAD_DIM), f32), -6.0, 6.0) * D ** (-0.5)
    return jnp.clip(values, -1.0, 1.0).astype(jnp.bfloat16)


def steps_of(stream_key, dims, cuts, least, top_value):
    def one(axis_at, blocks):
        steps = jax.random.uniform(jax.random.fold_in(jax.random.fold_in(stream_key, 6), axis_at), (blocks,), jnp.float32, least / len(cuts), top_value / len(cuts))
        return jnp.repeat(jnp.exp(steps), dims[axis_at] // blocks).reshape((-1,) + (1,) * (len(dims) - axis_at - 1))

    level = one(*cuts[0])
    for cut in cuts[1:]:
        level = level * one(*cut)
    return level


def split_up(number_of, total, reach, slope):
    weights = [(1 << 20) // math.isqrt(grade ** slope) + 1 for grade in range(2, number_of + 1)]
    rest, given = total - reach - (number_of - 1), [1] * (number_of - 1)
    while rest > 0:
        free = [i for i in range(number_of - 1) if given[i] < reach]
        whole, remaining = sum([weights[i] for i in free]), rest
        for i in free:
            addition = min(reach - given[i], max(1, remaining * weights[i] // whole), rest)
            given[i] = given[i] + addition
            rest = rest - addition
    return np.array([reach] + given)


def uneven(own_key, amount, total, limit, lean):
    if amount == 2:
        one = jax.random.randint(own_key, (), max(1, total - limit), min(limit, total - 1) + 1)
        return jnp.stack([one, total - one])
    sizes = jnp.asarray(split_up(amount, total, limit, lean), jnp.int32)
    twos = (amount - 1) // 2
    donor, receiver = sizes[1:1 + 2 * twos:2], sizes[2:2 + 2 * twos:2]
    slack = jnp.minimum(donor - 1, limit - receiver)
    shifted = jax.random.randint(jax.random.fold_in(own_key, 1), (twos,), 0, 1 << 20) % (slack + 1)
    sizes = sizes.at[1:1 + 2 * twos:2].set(donor - shifted).at[2:2 + 2 * twos:2].set(receiver + shifted)
    return sizes[jax.random.permutation(jax.random.fold_in(own_key, 2), amount)]


def centred(rng, dims, spread, most, cuts=(), kind=jnp.bfloat16):
    result = spread * jax.random.normal(rng, dims, jnp.float32)
    if cuts:
        result = result * steps_of(rng, dims, cuts, -0.22, 0.18)
    return jnp.clip(result, -most, most).astype(kind)


def setup_inputs(seed: int = 0, part: int = 0) -> dict:
    key_list = jax.random.split(jax.random.key(seed), 15)
    part_keys = jax.random.split(jax.random.fold_in(key_list[14], part), 15)
    tokens = draw_tokens(jax.random.fold_in(jax.random.fold_in(key_list[14], part), 71), part)
    gain = jnp.clip(1.0 + 0.18 * jax.random.normal(key_list[1], (D,), jnp.float32), 0.1, 1.9)
    w_query = draw_w_query(jax.random.fold_in(key_list[14], 71), part)
    w_key = draw_w_key(jax.random.fold_in(key_list[14], 71), part)
    w_value = centred(key_list[4], (D, KVW), D ** -0.5, 0.125, ((0, 8), (1, 2)))
    w_input = centred(key_list[5], (D, CW), D ** -0.5, 0.125, ((0, 8), (1, 2)))
    w_bgate = centred(key_list[6], (D, CW), D ** -0.5, 0.125, ((0, 8), (1, 2)))
    w_cgate = centred(key_list[7], (D, CW), D ** -0.5, 0.125, ((0, 8), (1, 2)))
    w_attn_out = centred(key_list[8], (QW, D), (max(1, QW // 128)) ** -0.5, 2.0, ((0, 8), (1, 2)))
    w_conv_out = centred(key_list[9], (CW, D), CW ** -0.5, 0.1875, ((0, 8), (1, 2)))
    sink_logit = jnp.clip(5.0 * jax.random.uniform(key_list[10], (Q_HEADS,), jnp.float32) ** steps_of(key_list[10], (Q_HEADS,), ((0, 2),), -0.2, 0.2), 0.0, 5.0)
    taps = centred(key_list[11], (3, CW), 3 ** -0.5, 3.5, ((1, 2),), jnp.float32)
    conv_bias = centred(key_list[12], (CW,), 1.0, 4.0, ((0, 2),), jnp.float32)
    documents = jnp.searchsorted(jnp.cumsum(uneven(part_keys[13], DOCS, TOKENS, 4 * TOK_DEV, 0)), jnp.arange(TOKENS), side="right").astype(jnp.int32)
    return {"tokens": tokens, "gain": gain, "w_query": w_query, "w_key": w_key, "w_value": w_value, "w_input": w_input, "w_bgate": w_bgate, "w_cgate": w_cgate, "w_attn_out": w_attn_out, "w_conv_out": w_conv_out, "sink_logit": sink_logit, "taps": taps, "conv_bias": conv_bias, "documents": documents}


EPS = 1e-06
THETA = 500000.0

def rotate(proj, positions, heads):
    rows = proj.shape[0]
    size = proj.shape[1] // heads
    half = size // 2
    freq = jnp.power(THETA, -(jnp.arange(half, dtype=jnp.float32) * (2.0 / size)))
    angle = positions.astype(jnp.float32)[:, None] * freq[None, :]
    cosine = jnp.cos(angle)[:, None, :]
    sine = jnp.sin(angle)[:, None, :]
    shaped = proj.reshape(rows, heads, size)
    first = shaped[..., :half]
    second = shaped[..., half:]
    turned = jnp.concatenate([first * cosine - second * sine, second * cosine + first * sine], axis=-1)
    return turned.reshape(rows, heads * size)

def sink_softmax(scores, allowed, sinks):
    masked = jnp.where(allowed, scores, -jnp.inf)
    top = jnp.maximum(lax.optimization_barrier(jnp.max(masked, axis=-1, keepdims=True)), sinks)
    expo = jnp.exp(masked - top)
    return expo / (lax.optimization_barrier(jnp.sum(expo, axis=-1, keepdims=True)) + jnp.exp(sinks - top))

def reference(tokens, gain, w_query, w_key, w_value, w_input, w_bgate, w_cgate, w_attn_out, w_conv_out, sink_logit, taps, conv_bias, documents):
    f32 = jnp.float32
    total = tokens.shape[0]
    xf = tokens.astype(f32)
    inv = lax.rsqrt(lax.optimization_barrier(jnp.sum(xf * xf, axis=1)) / D + EPS)[:, None]
    scaled = (xf * gain[None, :]).astype(jnp.bfloat16)
    qp = jnp.dot(scaled, w_query, preferred_element_type=f32) * inv
    kp = jnp.dot(scaled, w_key, preferred_element_type=f32) * inv
    vp = jnp.dot(scaled, w_value, preferred_element_type=f32) * inv
    upr = jnp.dot(scaled, w_input, preferred_element_type=f32) * inv
    bpr = jnp.dot(scaled, w_bgate, preferred_element_type=f32) * inv
    cpr = jnp.dot(scaled, w_cgate, preferred_element_type=f32) * inv
    positions = jnp.arange(total, dtype=jnp.int32)
    query = rotate(qp, positions, Q_HEADS).astype(jnp.bfloat16)
    keys = rotate(kp, positions, KV_HEADS).astype(jnp.bfloat16).reshape(total, KV_HEADS, HEAD_DIM)
    values = vp.astype(jnp.bfloat16).reshape(total, KV_HEADS, HEAD_DIM)
    groups = Q_HEADS // KV_HEADS
    sinks = sink_logit.astype(f32).reshape(KV_HEADS, groups, 1, 1)
    key_pad = jnp.pad(keys, ((WINDOW, WINDOW), (0, 0), (0, 0)))
    val_pad = jnp.pad(values, ((WINDOW, WINDOW), (0, 0), (0, 0)))
    doc_pad = jnp.pad(documents, (WINDOW, WINDOW), constant_values=-1)
    block = math.gcd(total, 512)
    span = block + 2 * WINDOW

    def one_block(index):
        begin = (index * block).astype(jnp.int32)
        qb = lax.dynamic_slice_in_dim(query, begin, block, 0).reshape(block, KV_HEADS, groups, HEAD_DIM)
        kb = lax.dynamic_slice_in_dim(key_pad, begin, span, 0)
        vb = lax.dynamic_slice_in_dim(val_pad, begin, span, 0)
        qdoc = lax.dynamic_slice_in_dim(documents, begin, block, 0)
        kdoc = lax.dynamic_slice_in_dim(doc_pad, begin, span, 0)
        qpos = begin + jnp.arange(block, dtype=jnp.int32)
        kpos = begin - WINDOW + jnp.arange(span, dtype=jnp.int32)
        scores = jnp.einsum('qhgd,khd->hgqk', qb.astype(f32), kb.astype(f32)) * HEAD_DIM ** (-0.5)
        allowed = (jnp.abs(qpos[:, None] - kpos[None, :]) <= WINDOW) & (qdoc[:, None] == kdoc[None, :])
        allowed = allowed & (kpos >= 0)[None, :] & (kpos < total)[None, :]
        weight = sink_softmax(scores, allowed, sinks).astype(jnp.bfloat16)
        out = jnp.einsum('hgqk,khd->qhgd', weight.astype(f32), vb.astype(f32))
        return out.astype(jnp.bfloat16).reshape(block, Q_HEADS * HEAD_DIM)
    attended = lax.map(one_block, jnp.arange(total // block, dtype=jnp.int32)).reshape(total, Q_HEADS * HEAD_DIM)
    carried = (cpr * upr).astype(jnp.bfloat16)
    car_pad = jnp.pad(carried, ((1, 1), (0, 0)))
    doc_near = jnp.pad(documents, (1, 1), constant_values=-1)
    conv = jnp.zeros((total, CW), f32)
    for tap in range(3):
        same = (doc_near[tap:tap + total] == documents)[:, None]
        conv = conv + jnp.where(same, car_pad[tap:tap + total].astype(f32) * taps[tap][None, :], 0.0)
    convolved = (bpr * (conv + conv_bias[None, :])).astype(jnp.bfloat16)
    mixed = jnp.dot(attended, w_attn_out, preferred_element_type=f32) + jnp.dot(convolved, w_conv_out, preferred_element_type=f32)
    return mixed.astype(jnp.bfloat16)
```

```python
import jax
import jax.numpy as jnp
from jax import lax
from jax.experimental import pallas as pl
from jax.experimental.pallas import tpu as pltpu
from jax.sharding import PartitionSpec as P

HEAD_DIM = 64
WINDOW = 128


EPS = 1e-06
THETA = 500000.0


def extended(cells, sides, width):
    for axis, dim in sides:
        count = lax.axis_size(axis)
        ends = count - 1
        head = lax.slice_in_dim(cells, 0, width, axis=dim)
        tail = lax.slice_in_dim(cells, cells.shape[dim] - width, cells.shape[dim], axis=dim)
        cells = jnp.concatenate(
            [
                lax.ppermute(tail, axis, [(i, (i + 1) % count) for i in range(ends)]),
                cells,
                lax.ppermute(head, axis, [((i + 1) % count, i) for i in range(ends)]),
            ],
            axis=dim,
        )
    return cells


def rotate(proj, positions, heads):
    rows = proj.shape[0]
    size = proj.shape[1] // heads
    half = size // 2
    freq = jnp.power(THETA, -(jnp.arange(half, dtype=jnp.float32) * (2.0 / size)))
    angle = positions.astype(jnp.float32)[:, None] * freq[None, :]
    cosine = jnp.cos(angle)[:, None, :]
    sine = jnp.sin(angle)[:, None, :]
    shaped = proj.reshape(rows, heads, size)
    first = shaped[..., :half]
    second = shaped[..., half:]
    turned = jnp.concatenate(
        [first * cosine - second * sine, second * cosine + first * sine], axis=-1
    )
    return turned.reshape(rows, heads * size)


def sink_softmax(scores, allowed, sinks):
    masked = jnp.where(allowed, scores, -jnp.inf)
    top = jnp.maximum(jnp.max(masked, axis=-1, keepdims=True), sinks)
    expo = jnp.exp(masked - top)
    return expo / (jnp.sum(expo, axis=-1, keepdims=True) + jnp.exp(sinks - top))


CORES = 2
FEW_CHIPS = 8


def swap_parts(cells, axis):
    count = lax.axis_size(axis)
    return [cells] + [
        lax.ppermute(cells, axis, [(i, (i + d) % count) for i in range(count)])
        for d in range(1, count)
    ]


def shifted(cells, t, chips):
    perm = [(i, ((i // CORES + t) % chips) * CORES + i % CORES) for i in range(chips * CORES)]
    return lax.ppermute(cells, "sp", perm)


def gathered(shard):
    chips = lax.axis_size("sp") // CORES
    copies = lax.axis_size("grp")
    if chips > FEW_CHIPS:
        whole = lax.all_gather(shard, "sp", axis=0, tiled=True)
        return jnp.split(whole, 2)
    piece = shard.shape[0] // copies
    mine = lax.dynamic_slice_in_dim(shard, lax.axis_index("grp") * piece, piece, 0)
    far = jnp.concatenate([shifted(mine, t, chips) for t in range(1, chips)], axis=0)
    whole = jnp.concatenate([shard] + swap_parts(far, "grp"), axis=0)
    count = chips * CORES
    other = lax.ppermute(whole, "sp", [(i, i ^ 1) for i in range(count)])
    return whole, other


def relative_blocks():
    chips = lax.axis_size("sp") // CORES
    copies = lax.axis_size("grp")
    if chips > FEW_CHIPS:
        return [(s, j) for s in range(chips * CORES) for j in range(copies)]
    grp = lax.axis_index("grp")
    spot = lax.axis_index("sp")
    chip, core = spot // CORES, spot % CORES
    order = []
    for k in range(CORES):
        c = (core + k) % CORES
        order += [(chip * CORES + c, j) for j in range(copies)]
        for d in range(copies):
            for t in range(1, chips):
                order.append((((chip - t) % chips) * CORES + c, (grp - d) % copies))
    return order


def by_owner(feature, part, parts):
    return ((lax.axis_index("tp") - feature // part) % parts) * part + feature % part


def scale_kernel(at_ref, raw_at_ref, tok_ref, gain_ref, out_ref, sq_ref, *, size):
    total = None
    for i in range(out_ref.shape[1] // size):
        cols = tok_ref[:, pl.ds(pl.multiple_of(at_ref[i], size), size)].astype(jnp.float32)
        factor = gain_ref[:, pl.ds(pl.multiple_of(raw_at_ref[i], size), size)]
        out_ref[:, i * size : (i + 1) * size] = (cols * factor).astype(out_ref.dtype)
        square = cols * cols
        total = square if total is None else total + square
    sq_ref[...] = jnp.broadcast_to(jnp.sum(total, axis=1, keepdims=True), sq_ref.shape)


def pick_kernel(at_ref, src_ref, out_ref, *, size):
    for i in range(out_ref.shape[1] // size):
        out_ref[:, i * size : (i + 1) * size] = src_ref[:, pl.ds(pl.multiple_of(at_ref[i], size), size)]


def row_tile(rows):
    return rows // 4 if rows % 64 == 0 else rows


def scaled_blocks(tok, gain, at, raw_at, size):
    rows, width = tok.shape
    if size % 128:
        wide = tok.astype(jnp.float32)
        out = [
            (
                lax.dynamic_slice_in_dim(wide, at[i], size, 1)
                * lax.dynamic_slice_in_dim(gain, raw_at[i], size, 0)[None, :]
            ).astype(tok.dtype)
            for i in range(width // size)
        ]
        return jnp.concatenate(out, axis=1), jnp.sum(wide * wide, axis=1, keepdims=True)
    tile = row_tile(rows)
    out, squares = pl.pallas_call(
        lambda *refs: scale_kernel(*refs, size=size),
        out_shape=(
            jax.ShapeDtypeStruct((rows, width), tok.dtype),
            jax.ShapeDtypeStruct((rows, 128), jnp.float32),
        ),
        grid_spec=pltpu.PrefetchScalarGridSpec(
            num_scalar_prefetch=2,
            grid=(rows // tile,),
            in_specs=[
                pl.BlockSpec((tile, width), lambda r, *_: (r, 0)),
                pl.BlockSpec((1, width), lambda r, *_: (0, 0)),
            ],
            out_specs=[
                pl.BlockSpec((tile, width), lambda r, *_: (r, 0)),
                pl.BlockSpec((tile, 128), lambda r, *_: (r, 0)),
            ],
        ),
        name="scale_blocks",
    )(at, raw_at, tok, gain[None, :])
    return out, squares[:, :1]


def picked_blocks(src, at, size):
    rows, width = src.shape
    if size % 128:
        return jnp.concatenate(
            [lax.dynamic_slice_in_dim(src, at[i], size, 1) for i in range(width // size)], axis=1
        )
    tile = row_tile(rows)
    return pl.pallas_call(
        lambda *refs: pick_kernel(*refs, size=size),
        out_shape=jax.ShapeDtypeStruct((rows, width), src.dtype),
        grid_spec=pltpu.PrefetchScalarGridSpec(
            num_scalar_prefetch=1,
            grid=(rows // tile,),
            in_specs=[pl.BlockSpec((tile, width), lambda r, *_: (r, 0))],
            out_specs=pl.BlockSpec((tile, width), lambda r, *_: (r, 0)),
        ),
        name="pick_blocks",
    )(at, src)


def product(left, pair):
    cut = pair[0].shape[0]
    f32 = jnp.float32
    return jnp.dot(left[:, :cut], pair[0], preferred_element_type=f32) + jnp.dot(
        left[:, cut:], pair[1], preferred_element_type=f32
    )


def local(
    tokens,
    gain,
    w_query,
    w_key,
    w_value,
    w_input,
    w_bgate,
    w_cgate,
    w_attn_out,
    w_conv_out,
    sink_logit,
    taps,
    conv_bias,
    documents,
):
    f32 = jnp.float32
    bf16 = jnp.bfloat16
    rows, part = tokens.shape
    tp_count = lax.axis_size("tp")
    sp_count = lax.axis_size("sp")
    width = part * tp_count
    head_dim = HEAD_DIM
    q_local = w_query.shape[1] // head_dim
    kv_local = w_key.shape[1] // head_dim
    groups = q_local // kv_local
    copies = lax.axis_size("grp")
    tok = jnp.concatenate(swap_parts(tokens, "tp"), axis=1)
    g_qkv = gathered(jnp.concatenate([w_query, w_key, w_value], axis=1))
    g_uc = gathered(jnp.concatenate([w_input, w_cgate], axis=1))
    g_b = gathered(w_bgate)
    g_out = gathered(jnp.concatenate([w_attn_out, w_conv_out], axis=0))
    order = relative_blocks()
    shard_rows = w_query.shape[0]
    size = shard_rows // copies
    raw_at = [shard * shard_rows + j * size for shard, j in order]
    at = jnp.stack([by_owner(f, part, tp_count) for f in raw_at]).astype(jnp.int32)
    raw_at = jnp.stack(raw_at).astype(jnp.int32)
    scaled, squares = scaled_blocks(tok, gain, at, raw_at, size)
    inv = lax.rsqrt(squares / width + EPS)
    qkv = product(scaled, g_qkv)
    q_width = w_query.shape[1]
    kv_width = w_key.shape[1]
    q_acc = qkv[:, :q_width]
    k_acc = qkv[:, q_width : q_width + kv_width]
    v_acc = qkv[:, q_width + kv_width :]
    uc = product(scaled, g_uc)
    u_acc, c_acc = uc[:, : w_input.shape[1]], uc[:, w_input.shape[1] :]
    b_acc = product(scaled, g_b)
    positions = lax.axis_index("sp") * rows + jnp.arange(rows, dtype=jnp.int32)
    query = rotate(q_acc * inv, positions, q_local).astype(bf16)
    keys = rotate(k_acc * inv, positions, kv_local).astype(bf16)
    values = (v_acc * inv).astype(bf16)
    carried = (c_acc * inv * (u_acc * inv)).astype(bf16)
    bgate = b_acc * inv
    doc_row = documents.astype(f32).astype(bf16)[None, :]
    doc_ext = extended(doc_row, (("sp", 1),), WINDOW)[0].astype(f32)
    paired = jnp.concatenate([keys, values], axis=1)
    pair_ext = extended(paired, (("sp", 0),), WINDOW)
    carry_ext = extended(carried, (("sp", 0),), 1)
    key_width = kv_local * head_dim
    key_ext = pair_ext[:, :key_width].reshape(-1, kv_local, head_dim)
    val_ext = pair_ext[:, key_width:].reshape(-1, kv_local, head_dim)
    key_doc = doc_ext
    own_doc = documents.astype(f32)
    key_pos = positions[0] - WINDOW + jnp.arange(rows + 2 * WINDOW, dtype=jnp.int32)
    total = sp_count * rows
    sinks = sink_logit.reshape(kv_local, groups, 1, 1)
    block = rows // 2
    outputs = []
    for begin in range(0, rows, block):
        span = block + 2 * WINDOW
        q_block = query[begin : begin + block].reshape(block, kv_local, groups, head_dim)
        k_block = key_ext[begin : begin + span]
        v_block = val_ext[begin : begin + span]
        q_pos = positions[begin : begin + block]
        k_pos = key_pos[begin : begin + span]
        scores = jnp.einsum(
            "qhgd,khd->hgqk", q_block, k_block, preferred_element_type=f32
        ) * head_dim ** (-0.5)
        allowed = jnp.abs(q_pos[:, None] - k_pos[None, :]) <= WINDOW
        allowed = allowed & (
            own_doc[begin : begin + block, None] == key_doc[None, begin : begin + span]
        )
        allowed = allowed & (k_pos >= 0)[None, :] & (k_pos < total)[None, :]
        weight = sink_softmax(scores, allowed, sinks).astype(bf16)
        result = jnp.einsum("hgqk,khd->qhgd", weight, v_block, preferred_element_type=f32)
        outputs.append(result.astype(bf16).reshape(block, q_local * head_dim))
    attended = jnp.concatenate(outputs, axis=0)
    near_doc = doc_ext[WINDOW - 1 : WINDOW + rows + 1]
    conv = jnp.zeros((rows, carried.shape[1]), f32)
    for tap in range(3):
        same = (near_doc[tap : tap + rows] == near_doc[1 : rows + 1])[:, None]
        conv = conv + jnp.where(
            same, carry_ext[tap : tap + rows].astype(f32) * taps[tap][None, :], 0.0
        )
    convolved = (bgate * (conv + conv_bias[None, :])).astype(bf16)
    mixers = jnp.concatenate(swap_parts(attended, "tp") + swap_parts(convolved, "tp"), axis=1)
    out_rows = w_attn_out.shape[0]
    q_part, c_part = attended.shape[1], convolved.shape[1]
    span = 2 * out_rows // copies
    places = []
    for shard, j in order:
        spot = j * span
        which, offset = spot // out_rows, spot % out_rows
        feature = shard * out_rows + offset
        places.append(
            jnp.where(
                which == 0,
                by_owner(feature, q_part, tp_count),
                q_part * tp_count + by_owner(feature, c_part, tp_count),
            )
        )
    picked = picked_blocks(mixers, jnp.stack(places).astype(jnp.int32), span)
    return product(picked, g_out).astype(bf16)


def solution(mesh):
    placed = (
        P(("grp", "sp"), "tp"),
        P(),
        P("sp", "tp"),
        P("sp", "tp"),
        P("sp", "tp"),
        P("sp", "tp"),
        P("sp", "tp"),
        P("sp", "tp"),
        P("sp", "tp"),
        P("sp", "tp"),
        P("tp"),
        P(None, "tp"),
        P("tp"),
        P(("grp", "sp")),
    )
    return jax.shard_map(
        local, mesh=mesh, in_specs=placed, out_specs=P(("grp", "sp"), "tp"), check_vma=False
    )
```

```python
import jax
import jax.numpy as jnp
from jax import lax
from jax.experimental import pallas as pl
from jax.experimental.pallas import tpu as pltpu
from jax.sharding import PartitionSpec as P

HEAD_DIM = 64
WINDOW = 128


EPS = 1e-06
THETA = 500000.0


def extended(cells, sides, width):
    for axis, dim in sides:
        count = lax.axis_size(axis)
        ends = count - 1
        head = lax.slice_in_dim(cells, 0, width, axis=dim)
        tail = lax.slice_in_dim(cells, cells.shape[dim] - width, cells.shape[dim], axis=dim)
        cells = jnp.concatenate(
            [
                lax.ppermute(tail, axis, [(i, (i + 1) % count) for i in range(ends)]),
                cells,
                lax.ppermute(head, axis, [((i + 1) % count, i) for i in range(ends)]),
            ],
            axis=dim,
        )
    return cells


def rotate(proj, positions, heads):
    rows = proj.shape[0]
    size = proj.shape[1] // heads
    half = size // 2
    freq = jnp.power(THETA, -(jnp.arange(half, dtype=jnp.float32) * (2.0 / size)))
    angle = positions.astype(jnp.float32)[:, None] * freq[None, :]
    cosine = jnp.cos(angle)[:, None, :]
    sine = jnp.sin(angle)[:, None, :]
    shaped = proj.reshape(rows, heads, size)
    first = shaped[..., :half]
    second = shaped[..., half:]
    turned = jnp.concatenate(
        [first * cosine - second * sine, second * cosine + first * sine], axis=-1
    )
    return turned.reshape(rows, heads * size)


def sink_softmax(scores, allowed, sinks):
    masked = jnp.where(allowed, scores, -jnp.inf)
    top = jnp.maximum(jnp.max(masked, axis=-1, keepdims=True), sinks)
    expo = jnp.exp(masked - top)
    return expo / (jnp.sum(expo, axis=-1, keepdims=True) + jnp.exp(sinks - top))


CORES = 2
FEW_CHIPS = 8


def swap_parts(cells, axis):
    count = lax.axis_size(axis)
    return [cells] + [
        lax.ppermute(cells, axis, [(i, (i + d) % count) for i in range(count)])
        for d in range(1, count)
    ]


def shifted(cells, t, chips):
    perm = [(i, ((i // CORES + t) % chips) * CORES + i % CORES) for i in range(chips * CORES)]
    return lax.ppermute(cells, "sp", perm)


def join_kernel(*refs, spots, skip):
    out_ref = refs[-1]
    for ref, spot in zip(refs[skip:-1], spots):
        out_ref[spot : spot + ref.shape[0], :] = ref[...]


def joined(pieces, after=()):
    if pieces[0].shape[1] % 128 or any(p.shape[0] % 16 for p in pieces):
        return jnp.concatenate(pieces, axis=0)
    spots, rows = [], 0
    for piece in pieces:
        spots.append(rows)
        rows += piece.shape[0]
    vmem = pl.BlockSpec(memory_space=pltpu.VMEM)
    return pl.pallas_call(
        lambda *refs: join_kernel(*refs, spots=spots, skip=len(after)),
        out_shape=jax.ShapeDtypeStruct((rows, pieces[0].shape[1]), pieces[0].dtype),
        in_specs=[pl.BlockSpec(memory_space=pl.ANY)] * len(after) + [vmem] * len(pieces),
        out_specs=vmem,
        name="join_rows",
    )(*after, *pieces)


def spread(shard):
    chips = lax.axis_size("sp") // CORES
    piece = shard.shape[0] // lax.axis_size("grp")
    if chips > FEW_CHIPS:
        return []
    mine = lax.dynamic_slice_in_dim(shard, lax.axis_index("grp") * piece, piece, 0)
    out = []
    for t in range(1, chips):
        out.append(shifted(mine, t, chips))
    return out


def crossed(far, after=()):
    return swap_parts(joined(far, after), "grp") if far else []


def gathered(shard, parts, after=()):
    count = lax.axis_size("sp")
    if count // CORES > FEW_CHIPS:
        whole = lax.all_gather(shard, "sp", axis=0, tiled=True)
        return jnp.split(whole, 2)
    whole = joined([shard] + parts, after)
    return whole, lax.ppermute(whole, "sp", [(i, i ^ 1) for i in range(count)])


def relative_blocks():
    chips = lax.axis_size("sp") // CORES
    copies = lax.axis_size("grp")
    if chips > FEW_CHIPS:
        return [(s, j) for s in range(chips * CORES) for j in range(copies)]
    grp = lax.axis_index("grp")
    spot = lax.axis_index("sp")
    chip, core = spot // CORES, spot % CORES
    order = []
    for k in range(CORES):
        c = (core + k) % CORES
        order += [(chip * CORES + c, j) for j in range(copies)]
        for d in range(copies):
            for t in range(1, chips):
                order.append((((chip - t) % chips) * CORES + c, (grp - d) % copies))
    return order


def by_owner(feature, part, parts):
    return ((lax.axis_index("tp") - feature // part) % parts) * part + feature % part


def scale_kernel(at_ref, raw_at_ref, *refs, size):
    *tok_refs, gain_ref, out_ref, sq_ref = refs
    part = tok_refs[0].shape[1]
    for i in range(out_ref.shape[1] // size):
        factor = gain_ref[:, pl.ds(pl.multiple_of(raw_at_ref[i], size), size)]
        for p, tok_ref in enumerate(tok_refs):

            @pl.when(at_ref[i] // part == p)
            def _(tok_ref=tok_ref, factor=factor, i=i):
                cols = tok_ref[:, pl.ds(pl.multiple_of(at_ref[i] % part, size), size)]
                wide = cols.astype(jnp.float32) * factor
                out_ref[:, i * size : (i + 1) * size] = wide.astype(out_ref.dtype)

    total = None
    for tok_ref in tok_refs:
        for i in range(part // 128):
            cols = tok_ref[:, i * 128 : (i + 1) * 128].astype(jnp.float32)
            total = cols * cols if total is None else total + cols * cols
    sq_ref[...] = jnp.broadcast_to(jnp.sum(total, axis=1, keepdims=True), sq_ref.shape)


def pick_kernel(at_ref, *refs, size):
    *src_refs, out_ref = refs
    for i in range(out_ref.shape[1] // size):
        begin = 0
        for src_ref in src_refs:
            end = begin + src_ref.shape[1]

            @pl.when((at_ref[i] >= begin) & (at_ref[i] < end))
            def _(src_ref=src_ref, begin=begin, i=i):
                cols = pl.ds(pl.multiple_of(at_ref[i] - begin, size), size)
                out_ref[:, i * size : (i + 1) * size] = src_ref[:, cols]

            begin = end


def row_tile(rows):
    return rows // 4 if rows % 64 == 0 else rows


def scaled_blocks(toks, gain, at, raw_at, size):
    rows, width = toks[0].shape[0], gain.shape[0]
    tok = toks[0]
    if size % 128:
        wide = jnp.concatenate(toks, axis=1).astype(jnp.float32)
        out = [
            (
                lax.dynamic_slice_in_dim(wide, at[i], size, 1)
                * lax.dynamic_slice_in_dim(gain, raw_at[i], size, 0)[None, :]
            ).astype(tok.dtype)
            for i in range(width // size)
        ]
        return jnp.concatenate(out, axis=1), jnp.sum(wide * wide, axis=1, keepdims=True)
    tile = row_tile(rows)
    out, squares = pl.pallas_call(
        lambda *refs: scale_kernel(*refs, size=size),
        out_shape=(
            jax.ShapeDtypeStruct((rows, width), tok.dtype),
            jax.ShapeDtypeStruct((rows, 128), jnp.float32),
        ),
        grid_spec=pltpu.PrefetchScalarGridSpec(
            num_scalar_prefetch=2,
            grid=(rows // tile,),
            in_specs=[
                *(pl.BlockSpec((tile, t.shape[1]), lambda r, *_: (r, 0)) for t in toks),
                pl.BlockSpec((1, width), lambda r, *_: (0, 0)),
            ],
            out_specs=[
                pl.BlockSpec((tile, width), lambda r, *_: (r, 0)),
                pl.BlockSpec((tile, 128), lambda r, *_: (r, 0)),
            ],
        ),
        name="scale_blocks",
    )(at, raw_at, *toks, gain[None, :])
    return out, squares[:, :1]


def picked_blocks(srcs, at, size):
    rows, width = srcs[0].shape[0], sum(src.shape[1] for src in srcs)
    if size % 128:
        src = jnp.concatenate(srcs, axis=1)
        return jnp.concatenate(
            [lax.dynamic_slice_in_dim(src, at[i], size, 1) for i in range(width // size)], axis=1
        )
    tile = row_tile(rows)
    return pl.pallas_call(
        lambda *refs: pick_kernel(*refs, size=size),
        out_shape=jax.ShapeDtypeStruct((rows, width), srcs[0].dtype),
        grid_spec=pltpu.PrefetchScalarGridSpec(
            num_scalar_prefetch=1,
            grid=(rows // tile,),
            in_specs=[pl.BlockSpec((tile, src.shape[1]), lambda r, *_: (r, 0)) for src in srcs],
            out_specs=pl.BlockSpec((tile, width), lambda r, *_: (r, 0)),
        ),
        name="pick_blocks",
    )(at, *srcs)


def product(left, pair):
    cut = pair[0].shape[0]
    f32 = jnp.float32
    return jnp.dot(left[:, :cut], pair[0], preferred_element_type=f32) + jnp.dot(
        left[:, cut:], pair[1], preferred_element_type=f32
    )


def local(
    tokens,
    gain,
    w_query,
    w_key,
    w_value,
    w_input,
    w_bgate,
    w_cgate,
    w_attn_out,
    w_conv_out,
    sink_logit,
    taps,
    conv_bias,
    documents,
):
    f32 = jnp.float32
    bf16 = jnp.bfloat16
    rows, part = tokens.shape
    tp_count = lax.axis_size("tp")
    sp_count = lax.axis_size("sp")
    width = part * tp_count
    head_dim = HEAD_DIM
    q_local = w_query.shape[1] // head_dim
    kv_local = w_key.shape[1] // head_dim
    groups = q_local // kv_local
    copies = lax.axis_size("grp")
    toks = swap_parts(tokens, "tp")
    s_qkv = jnp.concatenate([w_query, w_key, w_value], axis=1)
    s_uc = jnp.concatenate([w_input, w_cgate], axis=1)
    s_out = jnp.concatenate([w_attn_out, w_conv_out], axis=0)
    far_qkv = spread(s_qkv)
    far_uc = spread(s_uc)
    far_b = spread(w_bgate)
    far_out = spread(s_out)
    y_qkv = crossed(far_qkv)
    y_uc = crossed(far_uc)
    g_qkv = gathered(s_qkv, y_qkv)
    order = relative_blocks()
    shard_rows = w_query.shape[0]
    size = shard_rows // copies
    raw_at = [shard * shard_rows + j * size for shard, j in order]
    at = jnp.stack([by_owner(f, part, tp_count) for f in raw_at]).astype(jnp.int32)
    raw_at = jnp.stack(raw_at).astype(jnp.int32)
    scaled, squares = scaled_blocks(toks, gain, at, raw_at, size)
    inv = lax.rsqrt(squares / width + EPS)
    qkv = product(scaled, g_qkv)
    q_width = w_query.shape[1]
    kv_width = w_key.shape[1]
    q_acc = qkv[:, :q_width]
    k_acc = qkv[:, q_width : q_width + kv_width]
    v_acc = qkv[:, q_width + kv_width :]
    positions = lax.axis_index("sp") * rows + jnp.arange(rows, dtype=jnp.int32)
    query = rotate(q_acc * inv, positions, q_local).astype(bf16)
    keys = rotate(k_acc * inv, positions, kv_local).astype(bf16)
    values = (v_acc * inv).astype(bf16)
    doc_row = documents.astype(f32).astype(bf16)[None, :]
    doc_ext = extended(doc_row, (("sp", 1),), WINDOW)[0].astype(f32)
    paired = jnp.concatenate([keys, values], axis=1)
    pair_ext = extended(paired, (("sp", 0),), WINDOW)
    g_uc = gathered(s_uc, y_uc, (paired,))
    y_b = crossed(far_b, (paired,))
    uc = product(scaled, g_uc)
    u_acc, c_acc = uc[:, : w_input.shape[1]], uc[:, w_input.shape[1] :]
    carried = (c_acc * inv * (u_acc * inv)).astype(bf16)
    carry_ext = extended(carried, (("sp", 0),), 1)
    key_width = kv_local * head_dim
    key_ext = pair_ext[:, :key_width].reshape(-1, kv_local, head_dim)
    val_ext = pair_ext[:, key_width:].reshape(-1, kv_local, head_dim)
    key_doc = doc_ext
    own_doc = documents.astype(f32)
    key_pos = positions[0] - WINDOW + jnp.arange(rows + 2 * WINDOW, dtype=jnp.int32)
    total = sp_count * rows
    sinks = sink_logit.reshape(kv_local, groups, 1, 1)
    block = rows // 2
    outputs = []
    for begin in range(0, rows, block):
        span = block + 2 * WINDOW
        q_block = query[begin : begin + block].reshape(block, kv_local, groups, head_dim)
        k_block = key_ext[begin : begin + span]
        v_block = val_ext[begin : begin + span]
        q_pos = positions[begin : begin + block]
        k_pos = key_pos[begin : begin + span]
        scores = jnp.einsum(
            "qhgd,khd->hgqk", q_block, k_block, preferred_element_type=f32
        ) * head_dim ** (-0.5)
        allowed = jnp.abs(q_pos[:, None] - k_pos[None, :]) <= WINDOW
        allowed = allowed & (
            own_doc[begin : begin + block, None] == key_doc[None, begin : begin + span]
        )
        allowed = allowed & (k_pos >= 0)[None, :] & (k_pos < total)[None, :]
        weight = sink_softmax(scores, allowed, sinks).astype(bf16)
        result = jnp.einsum("hgqk,khd->qhgd", weight, v_block, preferred_element_type=f32)
        outputs.append(result.astype(bf16).reshape(block, q_local * head_dim))
    attended = jnp.concatenate(outputs, axis=0)
    mixers = swap_parts(attended, "tp")
    y_out = crossed(far_out, (attended,))
    g_b = gathered(w_bgate, y_b, (attended,))
    bgate = product(scaled, g_b) * inv
    near_doc = doc_ext[WINDOW - 1 : WINDOW + rows + 1]
    conv = jnp.zeros((rows, carried.shape[1]), f32)
    for tap in range(3):
        same = (near_doc[tap : tap + rows] == near_doc[1 : rows + 1])[:, None]
        conv = conv + jnp.where(
            same, carry_ext[tap : tap + rows].astype(f32) * taps[tap][None, :], 0.0
        )
    convolved = (bgate * (conv + conv_bias[None, :])).astype(bf16)
    mixers += swap_parts(convolved, "tp")
    g_out = gathered(s_out, y_out, (convolved,))
    out_rows = w_attn_out.shape[0]
    q_part, c_part = attended.shape[1], convolved.shape[1]
    span = 2 * out_rows // copies
    places = []
    for shard, j in order:
        spot = j * span
        which, offset = spot // out_rows, spot % out_rows
        feature = shard * out_rows + offset
        places.append(
            jnp.where(
                which == 0,
                by_owner(feature, q_part, tp_count),
                q_part * tp_count + by_owner(feature, c_part, tp_count),
            )
        )
    picked = picked_blocks(mixers, jnp.stack(places).astype(jnp.int32), span)
    return product(picked, g_out).astype(bf16)


def solution(mesh):
    placed = (
        P(("grp", "sp"), "tp"),
        P(),
        P("sp", "tp"),
        P("sp", "tp"),
        P("sp", "tp"),
        P("sp", "tp"),
        P("sp", "tp"),
        P("sp", "tp"),
        P("sp", "tp"),
        P("sp", "tp"),
        P("tp"),
        P(None, "tp"),
        P("tp"),
        P(("grp", "sp")),
    )
    return jax.shard_map(
        local, mesh=mesh, in_specs=placed, out_specs=P(("grp", "sp"), "tp"), check_vma=False
    )
```

```python
import jax
import jax.numpy as jnp
from jax import lax
from jax.experimental import pallas as pl
from jax.experimental.pallas import tpu as pltpu
from jax.sharding import PartitionSpec as P

HEAD_DIM = 64
WINDOW = 128


EPS = 1e-06
THETA = 500000.0


def extended(cells, sides, width):
    for axis, dim in sides:
        count = lax.axis_size(axis)
        ends = count - 1
        head = lax.slice_in_dim(cells, 0, width, axis=dim)
        tail = lax.slice_in_dim(cells, cells.shape[dim] - width, cells.shape[dim], axis=dim)
        cells = jnp.concatenate(
            [
                lax.ppermute(tail, axis, [(i, (i + 1) % count) for i in range(ends)]),
                cells,
                lax.ppermute(head, axis, [((i + 1) % count, i) for i in range(ends)]),
            ],
            axis=dim,
        )
    return cells


def rotate(proj, positions, heads):
    rows = proj.shape[0]
    size = proj.shape[1] // heads
    half = size // 2
    freq = jnp.power(THETA, -(jnp.arange(half, dtype=jnp.float32) * (2.0 / size)))
    angle = positions.astype(jnp.float32)[:, None] * freq[None, :]
    cosine = jnp.cos(angle)[:, None, :]
    sine = jnp.sin(angle)[:, None, :]
    shaped = proj.reshape(rows, heads, size)
    first = shaped[..., :half]
    second = shaped[..., half:]
    turned = jnp.concatenate(
        [first * cosine - second * sine, second * cosine + first * sine], axis=-1
    )
    return turned.reshape(rows, heads * size)


def sink_softmax(scores, allowed, sinks):
    masked = jnp.where(allowed, scores, -jnp.inf)
    top = jnp.maximum(jnp.max(masked, axis=-1, keepdims=True), sinks)
    expo = jnp.exp(masked - top)
    return expo / (jnp.sum(expo, axis=-1, keepdims=True) + jnp.exp(sinks - top))


CORES = 2
FEW_CHIPS = 8


def swap_parts(cells, axis):
    count = lax.axis_size(axis)
    return [cells] + [
        lax.ppermute(cells, axis, [(i, (i + d) % count) for i in range(count)])
        for d in range(1, count)
    ]


def shifted(cells, t, chips):
    perm = [(i, ((i // CORES + t) % chips) * CORES + i % CORES) for i in range(chips * CORES)]
    return lax.ppermute(cells, "sp", perm)


def join_kernel(*refs, spots, skip):
    out_ref = refs[-1]
    for ref, spot in zip(refs[skip:-1], spots):
        out_ref[spot : spot + ref.shape[0], :] = ref[...]


def joined(pieces, after=()):
    if pieces[0].shape[1] % 128 or any(p.shape[0] % 16 for p in pieces):
        return jnp.concatenate(pieces, axis=0)
    spots, rows = [], 0
    for piece in pieces:
        spots.append(rows)
        rows += piece.shape[0]
    vmem = pl.BlockSpec(memory_space=pltpu.VMEM)
    return pl.pallas_call(
        lambda *refs: join_kernel(*refs, spots=spots, skip=len(after)),
        out_shape=jax.ShapeDtypeStruct((rows, pieces[0].shape[1]), pieces[0].dtype),
        in_specs=[pl.BlockSpec(memory_space=pl.ANY)] * len(after) + [vmem] * len(pieces),
        out_specs=vmem,
        name="join_rows",
    )(*after, *pieces)


def spread(shard):
    chips = lax.axis_size("sp") // CORES
    piece = shard.shape[0] // lax.axis_size("grp")
    if chips > FEW_CHIPS:
        return []
    mine = lax.dynamic_slice_in_dim(shard, lax.axis_index("grp") * piece, piece, 0)
    out = []
    for t in range(1, chips):
        out.append(shifted(mine, t, chips))
    return out


def crossed(far, after=()):
    return swap_parts(joined(far, after), "grp") if far else []


def gathered(shard, parts, after=()):
    count = lax.axis_size("sp")
    if count // CORES > FEW_CHIPS:
        whole = lax.all_gather(shard, "sp", axis=0, tiled=True)
        return jnp.split(whole, 2)
    whole = joined([shard] + parts, after)
    return whole, lax.ppermute(whole, "sp", [(i, i ^ 1) for i in range(count)])


def relative_blocks():
    chips = lax.axis_size("sp") // CORES
    copies = lax.axis_size("grp")
    if chips > FEW_CHIPS:
        return [(s, j) for s in range(chips * CORES) for j in range(copies)]
    grp = lax.axis_index("grp")
    spot = lax.axis_index("sp")
    chip, core = spot // CORES, spot % CORES
    order = []
    for k in range(CORES):
        c = (core + k) % CORES
        order += [(chip * CORES + c, j) for j in range(copies)]
        for d in range(copies):
            for t in range(1, chips):
                order.append((((chip - t) % chips) * CORES + c, (grp - d) % copies))
    return order


def by_owner(feature, part, parts):
    return ((lax.axis_index("tp") - feature // part) % parts) * part + feature % part


def scale_kernel(at_ref, raw_at_ref, *refs, size):
    *tok_refs, gain_ref, out_ref, sq_ref = refs
    part = tok_refs[0].shape[1]
    for i in range(out_ref.shape[1] // size):
        factor = gain_ref[:, pl.ds(pl.multiple_of(raw_at_ref[i], size), size)]
        for p, tok_ref in enumerate(tok_refs):

            @pl.when(at_ref[i] // part == p)
            def _(tok_ref=tok_ref, factor=factor, i=i):
                cols = tok_ref[:, pl.ds(pl.multiple_of(at_ref[i] % part, size), size)]
                wide = cols.astype(jnp.float32) * factor
                out_ref[:, i * size : (i + 1) * size] = wide.astype(out_ref.dtype)

    total = None
    for tok_ref in tok_refs:
        for i in range(part // 128):
            cols = tok_ref[:, i * 128 : (i + 1) * 128].astype(jnp.float32)
            total = cols * cols if total is None else total + cols * cols
    sq_ref[...] = jnp.broadcast_to(jnp.sum(total, axis=1, keepdims=True), sq_ref.shape)


def pick_kernel(at_ref, *refs, size):
    *src_refs, out_ref = refs
    for i in range(out_ref.shape[1] // size):
        begin = 0
        for src_ref in src_refs:
            end = begin + src_ref.shape[1]

            @pl.when((at_ref[i] >= begin) & (at_ref[i] < end))
            def _(src_ref=src_ref, begin=begin, i=i):
                cols = pl.ds(pl.multiple_of(at_ref[i] - begin, size), size)
                out_ref[:, i * size : (i + 1) * size] = src_ref[:, cols]

            begin = end


def row_tile(rows):
    return rows // 4 if rows % 64 == 0 else rows


def scaled_blocks(toks, gain, at, raw_at, size):
    rows, width = toks[0].shape[0], gain.shape[0]
    tok = toks[0]
    if size % 128:
        wide = jnp.concatenate(toks, axis=1).astype(jnp.float32)
        out = [
            (
                lax.dynamic_slice_in_dim(wide, at[i], size, 1)
                * lax.dynamic_slice_in_dim(gain, raw_at[i], size, 0)[None, :]
            ).astype(tok.dtype)
            for i in range(width // size)
        ]
        return jnp.concatenate(out, axis=1), jnp.sum(wide * wide, axis=1, keepdims=True)
    tile = row_tile(rows)
    out, squares = pl.pallas_call(
        lambda *refs: scale_kernel(*refs, size=size),
        out_shape=(
            jax.ShapeDtypeStruct((rows, width), tok.dtype),
            jax.ShapeDtypeStruct((rows, 128), jnp.float32),
        ),
        grid_spec=pltpu.PrefetchScalarGridSpec(
            num_scalar_prefetch=2,
            grid=(rows // tile,),
            in_specs=[
                *(pl.BlockSpec((tile, t.shape[1]), lambda r, *_: (r, 0)) for t in toks),
                pl.BlockSpec((1, width), lambda r, *_: (0, 0)),
            ],
            out_specs=[
                pl.BlockSpec((tile, width), lambda r, *_: (r, 0)),
                pl.BlockSpec((tile, 128), lambda r, *_: (r, 0)),
            ],
        ),
        name="scale_blocks",
    )(at, raw_at, *toks, gain[None, :])
    return out, squares[:, :1]


def picked_blocks(srcs, at, size):
    rows, width = srcs[0].shape[0], sum(src.shape[1] for src in srcs)
    if size % 128:
        src = jnp.concatenate(srcs, axis=1)
        return jnp.concatenate(
            [lax.dynamic_slice_in_dim(src, at[i], size, 1) for i in range(width // size)], axis=1
        )
    tile = row_tile(rows)
    return pl.pallas_call(
        lambda *refs: pick_kernel(*refs, size=size),
        out_shape=jax.ShapeDtypeStruct((rows, width), srcs[0].dtype),
        grid_spec=pltpu.PrefetchScalarGridSpec(
            num_scalar_prefetch=1,
            grid=(rows // tile,),
            in_specs=[pl.BlockSpec((tile, src.shape[1]), lambda r, *_: (r, 0)) for src in srcs],
            out_specs=pl.BlockSpec((tile, width), lambda r, *_: (r, 0)),
        ),
        name="pick_blocks",
    )(at, *srcs)


def product(left, pair):
    cut = pair[0].shape[0]
    f32 = jnp.float32
    return jnp.dot(left[:, :cut], pair[0], preferred_element_type=f32) + jnp.dot(
        left[:, cut:], pair[1], preferred_element_type=f32
    )


def local(
    tokens,
    gain,
    w_query,
    w_key,
    w_value,
    w_input,
    w_bgate,
    w_cgate,
    w_attn_out,
    w_conv_out,
    sink_logit,
    taps,
    conv_bias,
    documents,
):
    f32 = jnp.float32
    bf16 = jnp.bfloat16
    rows, part = tokens.shape
    tp_count = lax.axis_size("tp")
    sp_count = lax.axis_size("sp")
    width = part * tp_count
    head_dim = HEAD_DIM
    q_local = w_query.shape[1] // head_dim
    kv_local = w_key.shape[1] // head_dim
    groups = q_local // kv_local
    copies = lax.axis_size("grp")
    toks = swap_parts(tokens, "tp")
    s_qkv = jnp.concatenate([w_query, w_key, w_value], axis=1)
    s_uc = jnp.concatenate([w_input, w_cgate], axis=1)
    s_out = jnp.concatenate([w_attn_out, w_conv_out], axis=0)
    far_qkv = spread(s_qkv)
    far_uc = spread(s_uc)
    far_b = spread(w_bgate)
    far_out = spread(s_out)
    y_qkv = crossed(far_qkv)
    y_uc = crossed(far_uc)
    g_qkv = gathered(s_qkv, y_qkv)
    order = relative_blocks()
    shard_rows = w_query.shape[0]
    size = shard_rows // copies
    raw_at = [shard * shard_rows + j * size for shard, j in order]
    at = jnp.stack([by_owner(f, part, tp_count) for f in raw_at]).astype(jnp.int32)
    raw_at = jnp.stack(raw_at).astype(jnp.int32)
    scaled, squares = scaled_blocks(toks, gain, at, raw_at, size)
    inv = lax.rsqrt(squares / width + EPS)
    qkv = product(scaled, g_qkv)
    q_width = w_query.shape[1]
    kv_width = w_key.shape[1]
    q_acc = qkv[:, :q_width]
    k_acc = qkv[:, q_width : q_width + kv_width]
    v_acc = qkv[:, q_width + kv_width :]
    positions = lax.axis_index("sp") * rows + jnp.arange(rows, dtype=jnp.int32)
    query = rotate(q_acc * inv, positions, q_local).astype(bf16)
    keys = rotate(k_acc * inv, positions, kv_local).astype(bf16)
    values = (v_acc * inv).astype(bf16)
    doc_row = documents.astype(f32).astype(bf16)[None, :]
    doc_ext = extended(doc_row, (("sp", 1),), WINDOW)[0].astype(f32)
    paired = jnp.concatenate([keys, values], axis=1)
    pair_ext = extended(paired, (("sp", 0),), WINDOW)
    g_uc = gathered(s_uc, y_uc, (paired,))
    y_b = crossed(far_b, (inv,))
    g_b = gathered(w_bgate, y_b, (paired,))
    y_out = crossed(far_out, (paired,))
    uc = product(scaled, g_uc)
    u_acc, c_acc = uc[:, : w_input.shape[1]], uc[:, w_input.shape[1] :]
    carried = (c_acc * inv * (u_acc * inv)).astype(bf16)
    carry_ext = extended(carried, (("sp", 0),), 1)
    key_width = kv_local * head_dim
    key_ext = pair_ext[:, :key_width].reshape(-1, kv_local, head_dim)
    val_ext = pair_ext[:, key_width:].reshape(-1, kv_local, head_dim)
    key_doc = doc_ext
    own_doc = documents.astype(f32)
    key_pos = positions[0] - WINDOW + jnp.arange(rows + 2 * WINDOW, dtype=jnp.int32)
    total = sp_count * rows
    sinks = sink_logit.reshape(kv_local, groups, 1, 1)
    block = rows // 2
    outputs = []
    for begin in range(0, rows, block):
        span = block + 2 * WINDOW
        q_block = query[begin : begin + block].reshape(block, kv_local, groups, head_dim)
        k_block = key_ext[begin : begin + span]
        v_block = val_ext[begin : begin + span]
        q_pos = positions[begin : begin + block]
        k_pos = key_pos[begin : begin + span]
        scores = jnp.einsum(
            "qhgd,khd->hgqk", q_block, k_block, preferred_element_type=f32
        ) * head_dim ** (-0.5)
        allowed = jnp.abs(q_pos[:, None] - k_pos[None, :]) <= WINDOW
        allowed = allowed & (
            own_doc[begin : begin + block, None] == key_doc[None, begin : begin + span]
        )
        allowed = allowed & (k_pos >= 0)[None, :] & (k_pos < total)[None, :]
        weight = sink_softmax(scores, allowed, sinks).astype(bf16)
        result = jnp.einsum("hgqk,khd->qhgd", weight, v_block, preferred_element_type=f32)
        outputs.append(result.astype(bf16).reshape(block, q_local * head_dim))
    attended = jnp.concatenate(outputs, axis=0)
    mixers = swap_parts(attended, "tp")
    g_out = gathered(s_out, y_out, (attended,))
    bgate = product(scaled, g_b) * inv
    near_doc = doc_ext[WINDOW - 1 : WINDOW + rows + 1]
    conv = jnp.zeros((rows, carried.shape[1]), f32)
    for tap in range(3):
        same = (near_doc[tap : tap + rows] == near_doc[1 : rows + 1])[:, None]
        conv = conv + jnp.where(
            same, carry_ext[tap : tap + rows].astype(f32) * taps[tap][None, :], 0.0
        )
    convolved = (bgate * (conv + conv_bias[None, :])).astype(bf16)
    mixers += swap_parts(convolved, "tp")
    out_rows = w_attn_out.shape[0]
    q_part, c_part = attended.shape[1], convolved.shape[1]
    span = 2 * out_rows // copies
    places = []
    for shard, j in order:
        spot = j * span
        which, offset = spot // out_rows, spot % out_rows
        feature = shard * out_rows + offset
        places.append(
            jnp.where(
                which == 0,
                by_owner(feature, q_part, tp_count),
                q_part * tp_count + by_owner(feature, c_part, tp_count),
            )
        )
    picked = picked_blocks(mixers, jnp.stack(places).astype(jnp.int32), span)
    return product(picked, g_out).astype(bf16)


def solution(mesh):
    placed = (
        P(("grp", "sp"), "tp"),
        P(),
        P("sp", "tp"),
        P("sp", "tp"),
        P("sp", "tp"),
        P("sp", "tp"),
        P("sp", "tp"),
        P("sp", "tp"),
        P("sp", "tp"),
        P("sp", "tp"),
        P("tp"),
        P(None, "tp"),
        P("tp"),
        P(("grp", "sp")),
    )
    return jax.shard_map(
        local, mesh=mesh, in_specs=placed, out_specs=P(("grp", "sp"), "tp"), check_vma=False
    )
```
